32 devices in a mesh: fs: 8 (over z, y), tp: 4 (over x, core).
Axes of the slice: x: 2, y: 2, z: 4, core: 2. Of those that a mesh axis runs over, the one named last changes fastest.
Arguments:
- mixed: bfloat16 [12288, 2048], P(('fs', 'tp')), may hold values from -6 to 6
- residual: bfloat16 [12288, 2048], P(('fs', 'tp')), may hold values from -6 to 6
- mix_weight: bfloat16 [2048, 2048], P(('fs', 'tp')), may hold values from -0.125 to 0.125
- norm_gain: float32 [2048], replicated, may hold values from 0.1 to 1.9
- up_weight: bfloat16 [2048, 5504], P('fs', 'tp'), may hold values from -0.125 to 0.125
- gate_weight: bfloat16 [2048, 5504], P('fs', 'tp'), may hold values from -0.125 to 0.125
- conv_weight: float32 [3, 5504], P(None, 'tp'), may hold values from -3 to 3
- conv_bias: float32 [5504], P('tp'), may hold values from -3 to 3
- down_weight: bfloat16 [5504, 2048], P('tp', 'fs'), may hold values from -0.078125 to 0.078125
Outputs:
- output: bfloat16 [12288, 2048], P(('fs', 'tp'))
The draws below stay inside these ranges and needn't reach their ends.
All inputs are finite; a program needn't handle non-finite values.
Results may differ from the reference program's by a relative error of at most 0.012.
Values may be sent and summed in bfloat16 or wider, within the bound.
No kernel may reach another device: no remote copies, remote signals or barrier semaphores. Data moves between devices by JAX's collectives and lax.ppermute only.
A program may use at most 128 MiB of HBM per device.

```python
import jax
import jax.numpy as jnp
from jax import lax

D = 2048
DM = 2048
FF = 5504
TOK_DEV = 384
TOKENS = 12288
N_FS = 8
N_TP = 4


def block_levels(stream_key, dims, shards, smallest, top_value):
    factor_of = 1.0
    for axis_at, parts in shards:
        steps = jax.random.uniform(jax.random.fold_in(jax.random.fold_in(stream_key, 6), axis_at), (parts,), jnp.float32, smallest / len(shards), top_value / len(shards))
        factor_of = factor_of * jnp.repeat(jnp.exp(steps), dims[axis_at] // parts).reshape((-1,) + (1,) * (len(dims) - 1 - axis_at))
    return factor_of


def scatter_about(own_key, shape, width, bound, pieces=(), kind=jnp.bfloat16):
    loudness = block_levels(own_key, shape, pieces, -0.22, 0.18) if pieces else 1.0
    entries = jax.random.normal(own_key, shape, jnp.float32) * width * loudness
    return jnp.minimum(jnp.maximum(entries, -bound), bound).astype(kind)


def setup_inputs(seed: int = 0) -> dict:
    streams_of = jax.random.split(jax.random.key(seed), 10)
    return {
        "mixed": scatter_about(streams_of[0], (TOKENS, DM), 1.0, 6.0, ((0, 32),)),
        "residual": scatter_about(streams_of[1], (TOKENS, D), 1.0, 6.0, ((0, 32),)),
        "mix_weight": scatter_about(streams_of[2], (DM, D), DM ** -0.5, 0.125, ((0, 32),)),
        "norm_gain": jnp.clip(1.0 + 0.18 * jax.random.normal(streams_of[3], (D,), jnp.float32), 0.1, 1.9),
        "up_weight": scatter_about(streams_of[4], (D, FF), D ** -0.5, 0.125, ((0, 8), (1, 4))),
        "gate_weight": scatter_about(streams_of[5], (D, FF), D ** -0.5, 0.125, ((0, 8), (1, 4))),
        "conv_weight": scatter_about(streams_of[6], (3, FF), 0.577, 3.0, ((1, 4),), jnp.float32),
        "conv_bias": scatter_about(streams_of[7], (FF,), 0.5, 3.0, ((0, 4),), jnp.float32),
        "down_weight": scatter_about(streams_of[8], (FF, D), FF ** -0.5, 0.078125, ((0, 4), (1, 8))),
    }


norm_eps = 1e-06

def reference(mixed, residual, mix_weight, norm_gain, up_weight, gate_weight, conv_weight, conv_bias, down_weight):
    unit_block = FF // N_TP
    length = TOK_DEV * N_TP
    stream = (residual.astype(jnp.float32) + jnp.dot(mixed, mix_weight, preferred_element_type=jnp.float32)).astype(jnp.bfloat16)
    x_float = stream.astype(jnp.float32)
    normed = (x_float * lax.rsqrt(lax.optimization_barrier(jnp.mean(x_float * x_float, axis=-1, keepdims=True)) + norm_eps) * norm_gain).astype(jnp.bfloat16)

    def one_seq(pair):
        normed_seq, stream_seq = pair
        up_part = jnp.dot(normed_seq, up_weight, preferred_element_type=jnp.float32).astype(jnp.bfloat16)
        gate_part = jnp.dot(normed_seq, gate_weight, preferred_element_type=jnp.float32).astype(jnp.bfloat16)
        up_float = lax.optimization_barrier(up_part).astype(jnp.float32)
        padded = jnp.pad(up_float, ((2, 0), (0, 0)))
        smoothed = conv_bias + conv_weight[0] * padded[:-2] + conv_weight[1] * padded[1:-1] + conv_weight[2] * padded[2:]
        hidden = (jax.nn.gelu(smoothed) * gate_part.astype(jnp.float32)).astype(jnp.bfloat16)
        accum_sum = stream_seq.astype(jnp.float32)
        for index in range(N_TP):
            partial_value = jnp.dot(hidden[:, index * unit_block:(index + 1) * unit_block], down_weight[index * unit_block:(index + 1) * unit_block], preferred_element_type=jnp.float32).astype(jnp.bfloat16)
            accum_sum = accum_sum + lax.optimization_barrier(partial_value).astype(jnp.float32)
        return accum_sum.astype(jnp.bfloat16)
    result = lax.map(one_seq, (normed.reshape(N_FS, length, D), stream.reshape(N_FS, length, D)))
    return result.reshape(N_FS * length, D)
```

```python
import jax
import jax.numpy as jnp
from jax import lax
from jax.sharding import Mesh, PartitionSpec as P

norm_eps = 1e-06


def swap(value, axis):
    return lax.ppermute(value, axis, [(0, 1), (1, 0)])


def make_body(depth):
    ring = [(i, (i + 1) % depth) for i in range(depth)]

    def turn(value):
        return lax.ppermute(value, "z", ring)

    def body(
        mixed,
        residual,
        mix_weight,
        norm_gain,
        up_weight,
        gate_weight,
        conv_weight,
        conv_bias,
        down_weight,
    ):
        f32, bf16 = jnp.float32, jnp.bfloat16
        z, y, x, c = (lax.axis_index(name) for name in "zyxc")
        tok, width = residual.shape
        rows = mix_weight.shape[0]
        inner = mixed.shape[1]
        fs_rows = up_weight.shape[0]
        block = up_weight.shape[1]
        half = block // 2
        main = half // 128 * 128
        tail = half - main
        first = y == 0

        def halves(array, axis):
            def cut(lo, hi):
                return lax.slice_in_dim(array, lo, hi, axis=axis)

            a = jnp.concatenate([cut(0, main), cut(2 * main, 2 * main + tail)], axis)
            b = jnp.concatenate([cut(main, 2 * main), cut(2 * main + tail, block)], axis)
            return jnp.where(first, a, b), jnp.where(first, b, a)

        def join(a, b):
            return [
                a[:, :main],
                b[:, :main],
                a[:, main:],
                b[:, main:],
            ]

        zs = [mix_weight]
        for _ in range(depth - 1):
            zs.append(turn(zs[-1]))
        pieces = []
        for own in zs:
            over_y = swap(own, "y")
            pair = jnp.concatenate([own, over_y], 0)
            over_x = swap(pair, "x")
            quad = jnp.concatenate([pair, over_x], 0)
            pieces.append(jnp.concatenate([quad, swap(quad, "c")], 0))
        col = jnp.arange(inner)
        r = col % rows
        b = col // rows
        fy, fx, fc, k = b % 2, (b // 2) % 2, (b // 4) % 2, b // 8
        source = (((((z - k) % depth) * 2 + (y ^ fy)) * 2 + (x ^ fx)) * 2 + (c ^ fc)) * rows + r
        select = (jnp.arange(inner)[:, None] == source[None, :]).astype(bf16)
        mixed_rel = jnp.dot(mixed, select, preferred_element_type=f32).astype(bf16)
        summed = jnp.dot(mixed_rel, jnp.concatenate(pieces, 0), preferred_element_type=f32)
        stream = (residual.astype(f32) + summed).astype(bf16)
        x_float = stream.astype(f32)
        normed = (
            x_float
            * lax.rsqrt(jnp.mean(x_float * x_float, axis=-1, keepdims=True) + norm_eps)
            * norm_gain
        ).astype(bf16)

        up_mine, up_send = halves(up_weight, 1)
        gate_mine, gate_send = halves(gate_weight, 1)
        ug_mine = jnp.concatenate(join(up_mine, gate_mine), 1)
        ug_over = swap(jnp.concatenate(join(up_send, gate_send), 1), "y")
        down_mine, down_send = halves(down_weight, 0)
        down_over = swap(down_send, "y")
        ug = jnp.zeros((depth * 2 * fs_rows, 2 * half), bf16)
        a, o = ug_mine, ug_over
        for k in range(depth):
            base = ((z - k) % depth) * 2 * fs_rows
            ug = lax.dynamic_update_slice(ug, a, (base + y * fs_rows, 0))
            ug = lax.dynamic_update_slice(ug, o, (base + (1 - y) * fs_rows, 0))
            if k + 1 < depth:
                a, o = turn(a), turn(o)
        downs = [
            jnp.where(
                first,
                jnp.concatenate([down_mine, down_over], 1),
                jnp.concatenate([down_over, down_mine], 1),
            )
        ]
        for _ in range(depth - 1):
            downs.append(turn(downs[-1]))

        over_x = swap(normed, "x")
        over_y = swap(normed, "y")
        cut = tok // 2
        over_xy = jnp.concatenate([swap(over_x[:cut], "y"), swap(over_y[cut:], "x")], 0)
        place = x * 2 + c
        seqs = []
        for same, other in ((normed, over_x), (over_y, over_xy)):
            seq = jnp.zeros((4 * tok, width), bf16)
            for value, where in (
                (same, place),
                (other, place ^ 2),
                (swap(same, "c"), place ^ 1),
                (swap(other, "c"), place ^ 3),
            ):
                seq = lax.dynamic_update_slice(seq, value, (where * tok, 0))
            seqs.append(seq)

        taps, _ = halves(conv_weight, 1)
        bias, _ = halves(conv_bias, 0)

        def hidden_of(seq):
            both = jnp.dot(seq, ug, preferred_element_type=f32).astype(bf16)
            cols = ((0, main, main, 0), (2 * main, 2 * main + tail, tail, main))
            out = []
            for up_at, gate_at, n, tap_at in cols:
                up_part = both[:, up_at : up_at + n]
                gate_part = both[:, gate_at : gate_at + n]
                t = taps[:, tap_at : tap_at + n]
                padded = jnp.pad(up_part.astype(f32), ((2, 0), (0, 0)))
                smoothed = (
                    bias[tap_at : tap_at + n]
                    + t[0] * padded[:-2]
                    + t[1] * padded[1:-1]
                    + t[2] * padded[2:]
                )
                out.append((jax.nn.gelu(smoothed) * gate_part.astype(f32)).astype(bf16))
            return jnp.concatenate(out, 1)

        hidden = [hidden_of(seq) for seq in seqs]

        out = jnp.zeros((tok, width), bf16)
        span = 2 * down_weight.shape[1]
        mid = span // 2
        for k in range(depth):
            parts = [
                jnp.dot(h, downs[k], preferred_element_type=f32).astype(bf16).reshape(2, 2, tok, span)
                for h in hidden
            ]
            both = jnp.stack(parts)
            keep = lax.dynamic_index_in_dim(both, c, 2, keepdims=False)
            send = lax.dynamic_index_in_dim(both, 1 - c, 2, keepdims=False)
            q = (keep.astype(f32) + swap(send, "c").astype(f32)).astype(bf16)
            mine = lax.dynamic_index_in_dim(q, x, 1, keepdims=False)
            theirs = lax.dynamic_index_in_dim(q, 1 - x, 1, keepdims=False)
            got = swap(theirs[:, :, :mid], "x")
            a = (mine[:, :, :mid].astype(f32) + got.astype(f32)).astype(bf16)
            left = a[0].astype(f32) + swap(a[1], "y").astype(f32)
            got_m = swap(jnp.stack([mine[1, :, mid:], theirs[1, :, mid:]]), "y")
            b_mine = mine[0, :, mid:].astype(f32) + got_m[0].astype(f32)
            b_theirs = (theirs[0, :, mid:].astype(f32) + got_m[1].astype(f32)).astype(bf16)
            right = b_mine + swap(b_theirs, "x").astype(f32)
            at = ((z - k) % depth) * span
            total = jnp.concatenate([left, right], 1)
            old = lax.dynamic_slice(stream, (0, at), (tok, span)).astype(f32)
            out = lax.dynamic_update_slice(out, (old + total).astype(bf16), (0, at))
        return out

    return body


def plain_body(
    mixed,
    residual,
    mix_weight,
    norm_gain,
    up_weight,
    gate_weight,
    conv_weight,
    conv_bias,
    down_weight,
):
    f32, bf16 = jnp.float32, jnp.bfloat16
    mix_full = lax.all_gather(mix_weight, ("fs", "tp"), axis=0, tiled=True)
    summed = jnp.dot(mixed, mix_full, preferred_element_type=f32)
    stream = (residual.astype(f32) + summed).astype(bf16)
    x_float = stream.astype(f32)
    scale = lax.rsqrt(jnp.mean(x_float * x_float, axis=-1, keepdims=True) + norm_eps)
    normed = (x_float * scale * norm_gain).astype(bf16)
    up_full = lax.all_gather(up_weight, "fs", axis=0, tiled=True)
    gate_full = lax.all_gather(gate_weight, "fs", axis=0, tiled=True)
    seq = lax.all_gather(normed, "tp", axis=0, tiled=True)
    up_part = jnp.dot(seq, up_full, preferred_element_type=f32).astype(bf16)
    gate_part = jnp.dot(seq, gate_full, preferred_element_type=f32).astype(bf16)
    padded = jnp.pad(lax.optimization_barrier(up_part).astype(f32), ((2, 0), (0, 0)))
    smoothed = (
        conv_bias
        + conv_weight[0] * padded[:-2]
        + conv_weight[1] * padded[1:-1]
        + conv_weight[2] * padded[2:]
    )
    hidden = (jax.nn.gelu(smoothed) * gate_part.astype(f32)).astype(bf16)
    down_full = lax.all_gather(down_weight, "fs", axis=1, tiled=True)
    partial = jnp.dot(hidden, down_full, preferred_element_type=f32).astype(bf16)
    total = lax.psum_scatter(partial, "tp", scatter_dimension=0, tiled=True)
    return (x_float + total.astype(f32)).astype(bf16)


def solution(mesh):
    fs, tp = mesh.shape["fs"], mesh.shape["tp"]
    chips_x, chips_y = (
        len({device.coords[i] for device in mesh.devices.flat}) for i in (0, 1)
    )
    cores = tp // chips_x
    if (chips_x, chips_y, cores) == (2, 2, 2):
        depth = fs // chips_y
        mesh = Mesh(
            mesh.devices.reshape(depth, chips_y, chips_x, cores), ("z", "y", "x", "c")
        )
        fs_axes, tp_axes, body = ("z", "y"), ("x", "c"), make_body(depth)
    else:
        fs_axes, tp_axes, body = ("fs",), ("tp",), plain_body
    tokens = P(fs_axes + tp_axes, None)
    return jax.shard_map(
        body,
        mesh=mesh,
        in_specs=(
            tokens,
            tokens,
            tokens,
            P(),
            P(fs_axes, tp_axes),
            P(fs_axes, tp_axes),
            P(None, tp_axes),
            P(tp_axes),
            P(tp_axes, fs_axes),
        ),
        out_specs=tokens,
        check_vma=False,
    )
```
